32 devices in a mesh: tp: 16 (over z, y, x), dp: 2 (over core).
Axes of the slice: x: 2, y: 2, z: 4, core: 2. Of those that a mesh axis runs over, the one named last changes fastest.
Arguments:
- tokens: bfloat16 [256, 4096], P(None, 'dp'), may hold values from -20 to 20
- norm_gain: float32 [2, 4096], P(None, 'dp'), may hold values from 0.1 to 1.9
- receptance: bfloat16 [2, 4096, 1024], P(None, 'dp', 'tp'), may hold values from -0.09375 to 0.09375
- key_proj: bfloat16 [2, 4096, 1024], P(None, 'dp', 'tp'), may hold values from -0.09375 to 0.09375
- value_proj: bfloat16 [2, 4096, 1024], P(None, 'dp', 'tp'), may hold values from -0.09375 to 0.09375
- decay_proj: bfloat16 [2, 4096, 1024], P(None, 'dp', 'tp'), may hold values from -0.09375 to 0.09375
- rate_proj: bfloat16 [2, 4096, 1024], P(None, 'dp', 'tp'), may hold values from -0.09375 to 0.09375
- gate_proj: bfloat16 [2, 4096, 1024], P(None, 'dp', 'tp'), may hold values from -0.09375 to 0.09375
- decay_base: float32 [2, 1024], P(None, 'tp'), may hold values from -6 to 1
- group_gain: float32 [2, 1024], P(None, 'tp'), may hold values from 0.1 to 1.9
- output_proj: bfloat16 [2, 1024, 4096], P(None, 'tp', 'dp'), may hold values from -0.1875 to 0.1875
- state: float32 [2, 256, 16, 4096], P(None, 'dp', 'tp'), may hold values from -3 to 3
Outputs:
- next_tokens: bfloat16 [256, 4096], P(None, 'dp')
- new_state: float32 [2, 256, 16, 4096], P(None, 'dp', 'tp')
The draws below stay inside these ranges and needn't reach their ends.
All inputs are finite; a program needn't handle non-finite values.
Results may differ from the reference program's by a relative error of at most 0.0066.
Values may be sent and summed in bfloat16 or wider, within the bound.
No kernel may reach another device: no remote copies, remote signals or barrier semaphores. Data moves between devices by JAX's collectives and lax.ppermute only.
A program may use at most 64 MiB of HBM per device.

```python
import jax
import jax.numpy as jnp
from jax import lax

D = 4096
HEAD = 64
HEADS = 16
D_ATT = 1024
LAYERS = 2
BATCH = 256


def draw_tokens(key, part):
    base_key, row_key = jax.random.split(key)
    position = jnp.arange(D, dtype=jnp.float32) / D
    feature_scale = 0.4 + 1.6 * position
    row_scale = jnp.exp(jax.random.uniform(row_key, (BATCH, 1), jnp.float32, -0.6, 0.6))
    values = jnp.clip(jax.random.normal(base_key, (BATCH, D), jnp.float32), -5.0, 5.0)
    return (values * feature_scale[None, :] * row_scale).astype(jnp.bfloat16)


def block_levels(stream_key, shape, pieces, low, high):
    def one(axis_at, blocks):
        draws = jax.random.uniform(jax.random.fold_in(jax.random.fold_in(stream_key, 6), axis_at), (blocks,), jnp.float32, low / len(pieces), high / len(pieces))
        return jnp.repeat(jnp.exp(draws), shape[axis_at] // blocks).reshape((-1,) + (1,) * (len(shape) - axis_at - 1))

    level = one(*pieces[0])
    for cut in pieces[1:]:
        level = level * one(*cut)
    return level


def gaussian(stream_key, shape, deviation, limit, cuts=(), held_as=jnp.bfloat16):
    loudness = block_levels(stream_key, shape, cuts, -0.22, 0.18) if cuts else 1.0
    drawn = jax.random.normal(stream_key, shape, jnp.float32) * deviation * loudness
    return jnp.minimum(jnp.maximum(drawn, -limit), limit).astype(held_as)


def setup_inputs(seed: int = 0) -> dict:
    arg_keys = jax.random.split(jax.random.key(seed), 13)
    return {
        "tokens": draw_tokens(jax.random.fold_in(arg_keys[12], 71), 0),
        "norm_gain": jnp.clip(1.0 + 0.18 * jax.random.normal(arg_keys[1], (LAYERS, D), jnp.float32), 0.1, 1.9),
        "receptance": gaussian(arg_keys[2], (LAYERS, D, D_ATT), D ** -0.5, 0.09375, ((1, 2), (2, 16))),
        "key_proj": gaussian(arg_keys[3], (LAYERS, D, D_ATT), D ** -0.5, 0.09375, ((1, 2), (2, 16))),
        "value_proj": gaussian(arg_keys[4], (LAYERS, D, D_ATT), D ** -0.5, 0.09375, ((1, 2), (2, 16))),
        "decay_proj": gaussian(arg_keys[5], (LAYERS, D, D_ATT), D ** -0.5, 0.09375, ((1, 2), (2, 16))),
        "rate_proj": gaussian(arg_keys[6], (LAYERS, D, D_ATT), D ** -0.5, 0.09375, ((1, 2), (2, 16))),
        "gate_proj": gaussian(arg_keys[7], (LAYERS, D, D_ATT), D ** -0.5, 0.09375, ((1, 2), (2, 16))),
        "decay_base": jnp.clip(-6.0 + 7.0 * jax.random.uniform(arg_keys[8], (LAYERS, D_ATT), jnp.float32) ** block_levels(arg_keys[8], (LAYERS, D_ATT), ((1, 16),), -0.2, 0.2), -6.0, 1.0),
        "group_gain": jnp.clip(1.0 + 0.18 * jax.random.normal(arg_keys[9], (LAYERS, D_ATT), jnp.float32), 0.1, 1.9),
        "output_proj": gaussian(arg_keys[10], (LAYERS, D_ATT, D), D_ATT ** -0.5, 0.1875, ((1, 16), (2, 2))),
        "state": gaussian(arg_keys[11], (LAYERS, BATCH, HEADS, HEAD * HEAD), 0.5, 3.0, ((1, 2), (2, 16)), jnp.float32),
    }


norm_floor = 0.1
group_floor = 0.5

def recurrence(state_block, recept_heads, key_heads, value_heads, decay_heads, rate_heads):
    log_rate = -jax.nn.softplus(-decay_heads) - 0.5
    forget = jnp.exp(-jnp.exp(log_rate))
    learn_rate = jax.nn.sigmoid(rate_heads)
    unit_key = key_heads * lax.rsqrt(lax.optimization_barrier(jnp.sum(key_heads * key_heads, axis=-1, keepdims=True)) + 1.0)
    scaled = key_heads * learn_rate
    removed = jnp.einsum('bhvk,bhk->bhv', state_block, -unit_key, precision=lax.Precision.HIGHEST)
    updated = state_block * forget[:, :, None, :] + removed[..., None] * (unit_key * learn_rate)[:, :, None, :] + value_heads[..., None] * scaled[:, :, None, :]
    read_out = jnp.einsum('bhvk,bhk->bhv', updated, recept_heads, precision=lax.Precision.HIGHEST)
    centre = read_out - lax.optimization_barrier(jnp.mean(read_out, axis=-1, keepdims=True))
    normal = centre * lax.rsqrt(lax.optimization_barrier(jnp.mean(centre * centre, axis=-1, keepdims=True)) + group_floor)
    return (updated, normal)

def reference(tokens, norm_gain, receptance, key_proj, value_proj, decay_proj, rate_proj, gate_proj, decay_base, group_gain, output_proj, state):
    current = tokens
    finals = []
    for section_index in range(LAYERS):
        floats = current.astype(jnp.float32)
        squares = lax.optimization_barrier(jnp.sum(floats * floats, axis=1))
        inv_rms = lax.rsqrt(squares / D + norm_floor)
        normed = (floats * norm_gain[section_index]).astype(jnp.bfloat16)

        def by_head(weights):
            term = jnp.dot(normed, weights[section_index], preferred_element_type=jnp.float32)
            rounded = lax.optimization_barrier((inv_rms[:, None] * term).astype(jnp.bfloat16))
            return rounded.astype(jnp.float32).reshape(BATCH, HEADS, HEAD)
        decay_heads = by_head(decay_proj) + decay_base[section_index].reshape(1, HEADS, HEAD)
        updated, normal = recurrence(state[section_index].reshape(BATCH, HEADS, HEAD, HEAD), by_head(receptance), by_head(key_proj), by_head(value_proj), decay_heads, by_head(rate_proj))
        finals.append(updated.reshape(BATCH, HEADS, HEAD * HEAD))
        gate_value = jax.nn.sigmoid(by_head(gate_proj).reshape(BATCH, D_ATT))
        mixed_heads = (normal.reshape(BATCH, D_ATT) * group_gain[section_index] * gate_value).astype(jnp.bfloat16)
        branch = jnp.dot(mixed_heads, output_proj[section_index], preferred_element_type=jnp.float32)
        current = (floats + branch).astype(jnp.bfloat16)
    return (current, jnp.stack(finals))
```

```python
import functools

import jax
import jax.numpy as jnp
from jax import lax
from jax.experimental import pallas as pl
from jax.experimental.pallas import tpu as pltpu
from jax.sharding import PartitionSpec as P

LANES = 128
norm_floor = 0.1
group_floor = 0.5
F32, BF16 = jnp.float32, jnp.bfloat16


def project_body(pos_ref, *refs, pieces, heads_width):
    count = len(pieces)
    x_refs, (gain_ref, *w_refs), (own_ref, other_ref), (normed, acc) = (
        refs[:count], refs[count:count + 7], refs[count + 7:count + 9], refs[count + 9:])
    squares = jnp.zeros((acc.shape[0], 1), F32)
    if count == 1:
        floats = x_refs[0][...].astype(F32)
        squares = jnp.sum(floats * floats, axis=1, keepdims=True)
        normed[...] = (floats * gain_ref[...]).astype(BF16)
    else:
        inner = count
        for b in range(inner):
            for a in range(x_refs[b].shape[0]):
                chunk = (pos_ref[1] ^ a) * inner + (pos_ref[2] ^ b)
                width = x_refs[b].shape[2]
                at = pl.ds(pl.multiple_of(chunk * width, LANES), width)
                floats = x_refs[b][a].astype(F32)
                squares = squares + jnp.sum(floats * floats, axis=1, keepdims=True)
                normed[:, at] = (floats * gain_ref[:, at]).astype(BF16)
    weights = jnp.concatenate([w[...] for w in w_refs], axis=0)
    acc[:, :6 * heads_width] = lax.dot_general(
        normed[...], weights, (((1,), (1,)), ((), ())), preferred_element_type=F32)
    acc[:, 6 * heads_width:] = jnp.broadcast_to(squares, (acc.shape[0], LANES))
    rows = own_ref.shape[0]
    core = pos_ref[0]
    own_ref[...] = acc[pl.ds(pl.multiple_of(core * rows, 8), rows), :]
    other_ref[...] = acc[pl.ds(pl.multiple_of((1 - core) * rows, 8), rows), :]


def masks(pairs, head):
    i = lax.broadcasted_iota(jnp.int32, (LANES, LANES), 0)
    j = lax.broadcasted_iota(jnp.int32, (LANES, LANES), 1)
    halves = jnp.where((i // head) == (j // head), 1.0, 0.0).astype(BF16)
    s = lax.broadcasted_iota(jnp.int32, (pairs, LANES), 0)
    lane = lax.broadcasted_iota(jnp.int32, (pairs, LANES), 1)
    place = jnp.where((lane == 2 * s) | (lane == head + 2 * s + 1), 1.0, 0.0)
    return halves, place


def half_sums(product, halves):
    high = product.astype(BF16)
    low = (product - high.astype(F32)).astype(BF16)
    return (jnp.dot(high, halves, preferred_element_type=F32)
            + jnp.dot(low, halves, preferred_element_type=F32))


def head_body(own_ref, recv_ref, base_ref, gain_ref, s_ref, mixed_ref, vec_ref, *, head, width):
    rows, pairs, _ = s_ref.shape
    total = own_ref[...] + recv_ref[...]
    inv_rms = lax.rsqrt(total[:, 6 * head:6 * head + 1] / width + norm_floor)
    seen = (total[:, :6 * head] * inv_rms).astype(BF16).astype(F32)
    recept, key, value, decay, rate, gate = (seen[:, n * head:(n + 1) * head] for n in range(6))
    forget = jnp.exp(-jnp.exp(jnp.float32(-0.5)) * jax.nn.sigmoid(decay + base_ref[...]))
    learn = jax.nn.sigmoid(rate)
    unit = key * lax.rsqrt(jnp.sum(key * key, axis=-1, keepdims=True) + 1.0)
    scaled = key * learn
    taken = unit * learn
    back = jnp.sum(taken * recept, axis=-1, keepdims=True)
    fresh = jnp.sum(scaled * recept, axis=-1, keepdims=True)
    probe = forget * recept - back * unit

    def twice(t):
        return jnp.concatenate([t, t], axis=1)

    halves, place = masks(pairs, head)
    product = (s_ref[...] * twice(probe)[:, None, :]).reshape(rows * pairs, LANES)
    sums = half_sums(product, halves).reshape(rows, pairs, LANES)
    folded = jnp.sum(sums * place[None], axis=1)
    read = folded[:, :head] + folded[:, head:] + value * fresh
    centre = read - jnp.mean(read, axis=-1, keepdims=True)
    normal = centre * lax.rsqrt(jnp.mean(centre * centre, axis=-1, keepdims=True) + group_floor)
    mixed_ref[...] = (normal * gain_ref[...] * jax.nn.sigmoid(gate)).astype(BF16)
    vec_ref[...] = jnp.concatenate(
        [twice(forget), twice(-unit), twice(taken), twice(value), twice(scaled)], axis=1)


def update_body(*refs, head):
    vec_ref, s_ref, out_ref = refs[0], refs[1], refs[-1]
    rows, pairs, _ = s_ref.shape
    forget, away, taken, value, scaled = (
        vec_ref[:, n * LANES:(n + 1) * LANES][:, None, :] for n in range(5))
    halves, place = masks(pairs, head)
    state = s_ref[...]
    removed = half_sums((state * away).reshape(rows * pairs, LANES), halves)
    spread = (value * place[None]).reshape(rows * pairs, LANES).astype(BF16)
    values = jnp.dot(spread, halves, preferred_element_type=F32)
    shape = (rows, pairs, LANES)
    out_ref[...] = state * forget + removed.reshape(shape) * taken + values.reshape(shape) * scaled


def output_body(pos_ref, *refs, outer, inner):
    m_refs, w_refs = refs[:outer], refs[outer:2 * outer]
    own_ref, sends = refs[2 * outer], refs[2 * outer + 1:-1]
    acc = refs[-1]
    left = jnp.concatenate([m[...] for m in m_refs], axis=1)
    right = jnp.concatenate([w[...] for w in w_refs], axis=0)
    acc[...] = jnp.dot(left, right, preferred_element_type=F32)
    width = own_ref.shape[1]
    for b in range(inner):
        at = pl.ds(pl.multiple_of((pos_ref[2] ^ b) * width, LANES), width)
        if b == 0:
            own_ref[...] = acc[:, at]
        else:
            sends[b - 1][...] = acc[:, at].astype(BF16)


def assemble_body(pos_ref, *refs):
    out_ref, inner = refs[-1], len(refs) - 1
    for b in range(inner):
        for a in range(refs[b].shape[0]):
            chunk = (pos_ref[1] ^ a) * inner + (pos_ref[2] ^ b)
            width = refs[b].shape[2]
            out_ref[:, pl.ds(pl.multiple_of(chunk * width, LANES), width)] = refs[b][a]


SMEM = functools.partial(pl.BlockSpec, memory_space=pltpu.SMEM)
VMEM = functools.partial(pl.BlockSpec, memory_space=pltpu.VMEM)


def whole(shape):
    return pl.BlockSpec(shape, lambda i: (0,) * len(shape))


def layer_of(array, layer):
    return pl.BlockSpec((None,) + array.shape[1:], lambda i: (layer,) + (0,) * (array.ndim - 1))


def shards(tp, dp, tokens, norm_gain, receptance, key_proj, value_proj, decay_proj, rate_proj,
           gate_proj, decay_base, group_gain, output_proj, state):
    inner = 4 if tp % 4 == 0 else tp
    outer = tp // inner
    layers, rows, _, cells = state.shape
    batch, local_width = tokens.shape
    head = decay_base.shape[1]
    pairs = cells // LANES
    width = local_width * dp
    me = lax.axis_index("tp")
    pos = jnp.stack([lax.axis_index("dp"), me // inner, me % inner]).astype(jnp.int32)
    far, near = me // inner, me % inner

    def over_far(t, s):
        return lax.ppermute(t, "tp", [(i, ((i // inner) ^ s) * inner + i % inner) for i in range(tp)])

    def over_near(t, s):
        return lax.ppermute(t, "tp", [(i, (i // inner) * inner + ((i % inner) ^ s)) for i in range(tp)])

    def swap(t):
        return lax.ppermute(t, "dp", [(i, i ^ 1) for i in range(dp)])

    projections = [jnp.swapaxes(w, 1, 2) for w in (
        receptance, key_proj, value_proj, decay_proj, rate_proj, gate_proj)]
    states = state.reshape(layers, rows, pairs, LANES)
    gains = norm_gain.reshape(layers, 1, local_width)
    bases = decay_base.reshape(layers, 1, head)
    group_gains = group_gain.reshape(layers, 1, head)

    band = local_width // outer
    chunk = band // inner
    bands = [lax.dynamic_slice_in_dim(output_proj, (far ^ s) * band, band, 2) for s in range(outer)]
    out_weights = [bands[0]] + [over_far(bands[s], s) for s in range(1, outer)]

    current = lax.dynamic_slice_in_dim(tokens, me * chunk, chunk, 1)
    gathered = (tokens,)
    new_states = None
    block = rows // 4
    vec_width = 5 * LANES
    for layer in range(layers):
        first = len(gathered) == 1
        sums_width = 6 * head + LANES
        own, other = pl.pallas_call(
            functools.partial(project_body, pieces=gathered, heads_width=head),
            grid=(1,),
            in_specs=[SMEM()] + [whole(g.shape) for g in gathered] + [layer_of(gains, layer)]
            + [layer_of(w, layer) for w in projections],
            out_specs=[whole((rows, sums_width))] * 2,
            out_shape=[jax.ShapeDtypeStruct((rows, sums_width), F32)] * 2,
            scratch_shapes=[pltpu.VMEM((batch, local_width), BF16), pltpu.VMEM((batch, sums_width), F32)],
            name=f"project{layer}",
        )(pos, *gathered, gains, *projections)
        received = swap(other)

        def row_block(w):
            return pl.BlockSpec((block, w), lambda i: (i, 0))

        state_block = pl.BlockSpec(
            (None, block, pairs, LANES), lambda i, layer=layer: (layer, i, 0, 0))
        small = pl.BlockSpec((None, 1, head), lambda i, layer=layer: (layer, 0, 0))
        mixed, vectors = pl.pallas_call(
            functools.partial(head_body, head=head, width=width),
            grid=(4,),
            in_specs=[row_block(sums_width), row_block(sums_width), small, small, state_block],
            out_specs=[row_block(head), row_block(vec_width)],
            out_shape=[jax.ShapeDtypeStruct((rows, head), BF16),
                       jax.ShapeDtypeStruct((rows, vec_width), F32)],
            name=f"heads{layer}",
        )(own, received, bases, group_gains, states)

        partner = swap(mixed)
        even = lax.axis_index("dp") == 0
        both = jnp.concatenate(
            [jnp.where(even, mixed, partner), jnp.where(even, partner, mixed)], axis=0)
        columns = [both] + [over_far(both, s) for s in range(1, outer)]

        previous = [] if new_states is None else [new_states]
        new_states = pl.pallas_call(
            functools.partial(update_body, head=head),
            grid=(4,),
            in_specs=[row_block(vec_width), state_block]
            + [pl.BlockSpec(memory_space=pl.ANY)] * len(previous),
            out_specs=state_block,
            out_shape=jax.ShapeDtypeStruct(states.shape, F32),
            input_output_aliases={2: 0} if previous else {},
            name=f"update{layer}",
        )(vectors, states, *previous)

        weights = [w[layer] for w in out_weights]
        mine, *sends = pl.pallas_call(
            functools.partial(output_body, outer=outer, inner=inner),
            grid=(1,),
            in_specs=[SMEM()] + [whole(c.shape) for c in columns] + [whole(w.shape) for w in weights],
            out_specs=[whole((batch, chunk))] * inner,
            out_shape=[jax.ShapeDtypeStruct((batch, chunk), F32)]
            + [jax.ShapeDtypeStruct((batch, chunk), BF16)] * (inner - 1),
            scratch_shapes=[pltpu.VMEM((batch, band), F32)],
            name=f"output{layer}",
        )(pos, *columns, *weights)
        total = current.astype(F32) + mine
        for s in range(1, inner):
            total = total + over_near(sends[s - 1], s).astype(F32)
        current = total.astype(BF16)
        stack = jnp.stack([current] + [over_far(current, s) for s in range(1, outer)])
        gathered = (stack,) + tuple(over_near(stack, s) for s in range(1, inner))

    final = pl.pallas_call(
        assemble_body,
        grid=(1,),
        in_specs=[SMEM()] + [whole(g.shape) for g in gathered],
        out_specs=whole((batch, local_width)),
        out_shape=jax.ShapeDtypeStruct((batch, local_width), BF16),
        name="assemble",
    )(pos, *gathered)
    return final, new_states.reshape(state.shape)


def recurrence(state_block, recept_heads, key_heads, value_heads, decay_heads, rate_heads):
    log_rate = -jax.nn.softplus(-decay_heads) - 0.5
    forget = jnp.exp(-jnp.exp(log_rate))
    learn_rate = jax.nn.sigmoid(rate_heads)
    unit_key = key_heads * lax.rsqrt(jnp.sum(key_heads * key_heads, axis=-1, keepdims=True) + 1.0)
    scaled = key_heads * learn_rate
    removed = jnp.einsum("bhvk,bhk->bhv", state_block, -unit_key, precision=lax.Precision.HIGHEST)
    updated = (
        state_block * forget[:, :, None, :]
        + removed[..., None] * (unit_key * learn_rate)[:, :, None, :]
        + value_heads[..., None] * scaled[:, :, None, :]
    )
    read_out = jnp.einsum("bhvk,bhk->bhv", updated, recept_heads, precision=lax.Precision.HIGHEST)
    centre = read_out - jnp.mean(read_out, axis=-1, keepdims=True)
    normal = centre * lax.rsqrt(jnp.mean(centre * centre, axis=-1, keepdims=True) + group_floor)
    return (updated, normal)


def plain_shards(
    tokens,
    norm_gain,
    receptance,
    key_proj,
    value_proj,
    decay_proj,
    rate_proj,
    gate_proj,
    decay_base,
    group_gain,
    output_proj,
    state,
):
    local_rows = state.shape[1]
    first_row = lax.axis_index("dp") * local_rows
    local_heads = state.shape[2]
    current = tokens
    width = tokens.shape[1] * lax.psum(1, "dp")
    head = decay_base.shape[1] // local_heads
    finals = []
    for section_index in range(state.shape[0]):
        floats = current.astype(jnp.float32)
        squares = jnp.sum(floats * floats, axis=1)
        normed = (floats * norm_gain[section_index]).astype(jnp.bfloat16)
        part_recept = jnp.dot(normed, receptance[section_index], preferred_element_type=jnp.float32)
        part_key = jnp.dot(normed, key_proj[section_index], preferred_element_type=jnp.float32)
        part_value = jnp.dot(normed, value_proj[section_index], preferred_element_type=jnp.float32)
        part_decay = jnp.dot(normed, decay_proj[section_index], preferred_element_type=jnp.float32)
        part_rate = jnp.dot(normed, rate_proj[section_index], preferred_element_type=jnp.float32)
        part_gate = jnp.dot(normed, gate_proj[section_index], preferred_element_type=jnp.float32)
        totals = lax.psum(squares, "dp")
        own_squares = lax.dynamic_slice_in_dim(totals, first_row, local_rows, 0)
        summed = (
            lax.psum_scatter(part_recept, "dp", scatter_dimension=0, tiled=True),
            lax.psum_scatter(part_key, "dp", scatter_dimension=0, tiled=True),
            lax.psum_scatter(part_value, "dp", scatter_dimension=0, tiled=True),
            lax.psum_scatter(part_decay, "dp", scatter_dimension=0, tiled=True),
            lax.psum_scatter(part_rate, "dp", scatter_dimension=0, tiled=True),
            lax.psum_scatter(part_gate, "dp", scatter_dimension=0, tiled=True),
        )
        inv_rms = lax.rsqrt(own_squares / width + norm_floor)

        def by_head(term):
            rounded = lax.optimization_barrier((inv_rms[:, None] * term).astype(jnp.bfloat16))
            return rounded.astype(jnp.float32).reshape(local_rows, local_heads, head)

        decay_heads = by_head(summed[3]) + decay_base[section_index].reshape(1, local_heads, head)
        updated, normal = recurrence(
            state[section_index].reshape(local_rows, local_heads, head, head),
            by_head(summed[0]),
            by_head(summed[1]),
            by_head(summed[2]),
            decay_heads,
            by_head(summed[4]),
        )
        finals.append(updated.reshape(local_rows, local_heads, state.shape[3]))
        gate_value = jax.nn.sigmoid(by_head(summed[5]).reshape(local_rows, local_heads * head))
        mixed_heads = (
            normal.reshape(local_rows, local_heads * head) * group_gain[section_index] * gate_value
        ).astype(jnp.bfloat16)
        weights_out = output_proj[section_index]

        def apply_out(piece, begin, weights_out=weights_out):
            return jnp.dot(piece, weights_out, preferred_element_type=jnp.float32)

        partial_out = apply_out(lax.all_gather(mixed_heads, "dp", axis=0, tiled=True), jnp.int32(0))
        total = lax.psum(partial_out, "tp")
        current = (floats + total).astype(jnp.bfloat16)
    return (current, jnp.stack(finals))


def solution(mesh):
    tp, dp = mesh.shape["tp"], mesh.shape["dp"]

    def body(*args):
        tokens, decay_base, state = args[0], args[8], args[11]
        chunks = tokens.shape[1] % (tp * LANES) == 0 and decay_base.shape[1] * 2 == LANES
        blocks = state.shape[1] % 64 == 0 and state.shape[2] == 1
        if dp == 2 and tp & (tp - 1) == 0 and tp % 4 == 0 and chunks and blocks:
            return shards(tp, dp, *args)
        return plain_shards(*args)

    return jax.shard_map(
        body,
        mesh=mesh,
        in_specs=(
            P(None, "dp"),
            P(None, "dp"),
            P(None, "dp", "tp"),
            P(None, "dp", "tp"),
            P(None, "dp", "tp"),
            P(None, "dp", "tp"),
            P(None, "dp", "tp"),
            P(None, "dp", "tp"),
            P(None, "tp"),
            P(None, "tp"),
            P(None, "tp", "dp"),
            P(None, "dp", "tp", None),
        ),
        out_specs=(P(None, "dp"), P(None, "dp", "tp", None)),
        check_vma=False,
    )
```

```python
import functools

import jax
import jax.numpy as jnp
from jax import lax
from jax.experimental import pallas as pl
from jax.experimental.pallas import tpu as pltpu
from jax.sharding import PartitionSpec as P

LANES = 128
norm_floor = 0.1
group_floor = 0.5
F32, BF16 = jnp.float32, jnp.bfloat16

COST = pl.CostEstimate(flops=20_000_000, transcendentals=0, bytes_accessed=8_000_000)


def project_body(pos_ref, *refs, count, layer, heads_width):
    x_refs, (gain_ref, *w_refs), (own_ref, other_ref), (normed, acc, weights, arrived) = (
        refs[:count], refs[count:count + 7], refs[-6:-4], refs[-4:])
    copies = [pltpu.make_async_copy(
        w.at[layer], weights.at[pl.ds(n * heads_width, heads_width)], arrived.at[n])
        for n, w in enumerate(w_refs)]
    for copy in copies:
        copy.start()
    squares = jnp.zeros((acc.shape[0], 1), F32)
    if count == 1:
        floats = x_refs[0][...].astype(F32)
        squares = jnp.sum(floats * floats, axis=1, keepdims=True)
        normed[...] = (floats * gain_ref[layer:layer + 1, :]).astype(BF16)
    else:
        inner = count
        for b in range(inner):
            for a in range(x_refs[b].shape[0]):
                chunk = (pos_ref[1] ^ a) * inner + (pos_ref[2] ^ b)
                width = x_refs[b].shape[2]
                at = pl.ds(pl.multiple_of(chunk * width, LANES), width)
                floats = x_refs[b][a].astype(F32)
                squares = squares + jnp.sum(floats * floats, axis=1, keepdims=True)
                normed[:, at] = (floats * gain_ref[layer:layer + 1, at]).astype(BF16)
    for copy in copies:
        copy.wait()
    acc[:, :6 * heads_width] = lax.dot_general(
        normed[...], weights[...], (((1,), (1,)), ((), ())), preferred_element_type=F32)
    acc[:, 6 * heads_width:] = jnp.broadcast_to(squares, (acc.shape[0], LANES))
    rows = own_ref.shape[0]
    if count == 1:
        core = pos_ref[0]
        own_ref[...] = acc[pl.ds(pl.multiple_of(core * rows, 8), rows), :]
        other_ref[...] = acc[pl.ds(pl.multiple_of((1 - core) * rows, 8), rows), :]
    else:
        own_ref[...] = acc[:rows, :]
        other_ref[...] = acc[rows:, :]


def masks(pairs, head):
    i = lax.broadcasted_iota(jnp.int32, (LANES, LANES), 0)
    j = lax.broadcasted_iota(jnp.int32, (LANES, LANES), 1)
    halves = jnp.where((i // head) == (j // head), 1.0, 0.0).astype(BF16)
    s = lax.broadcasted_iota(jnp.int32, (pairs, LANES), 0)
    lane = lax.broadcasted_iota(jnp.int32, (pairs, LANES), 1)
    place = jnp.where((lane == 2 * s) | (lane == head + 2 * s + 1), 1.0, 0.0)
    return halves, place


def half_sums(product, halves):
    high = product.astype(BF16)
    low = (product - high.astype(F32)).astype(BF16)
    return (jnp.dot(high, halves, preferred_element_type=F32)
            + jnp.dot(low, halves, preferred_element_type=F32))


def head_body(own_ref, recv_ref, base_ref, gain_ref, s_hbm, mixed_ref, vec_ref, s_ref, arrived,
              *, layer, head, width):
    rows, pairs, _ = s_ref.shape
    steps = arrived.shape[0]
    block = rows // steps
    copies = [pltpu.make_async_copy(
        s_hbm.at[layer, pl.ds(n * block, block)], s_ref.at[pl.ds(n * block, block)], arrived.at[n])
        for n in range(steps)]
    for copy in copies:
        copy.start()
    total = own_ref[...] + recv_ref[...]
    inv_rms = lax.rsqrt(total[:, 6 * head:6 * head + 1] / width + norm_floor)
    seen = (total[:, :6 * head] * inv_rms).astype(BF16).astype(F32)
    recept, key, value, decay, rate, gate = (seen[:, n * head:(n + 1) * head] for n in range(6))
    forget = jnp.exp(-jnp.exp(jnp.float32(-0.5)) * jax.nn.sigmoid(decay + base_ref[layer:layer + 1, :]))
    learn = jax.nn.sigmoid(rate)
    unit = key * lax.rsqrt(jnp.sum(key * key, axis=-1, keepdims=True) + 1.0)
    scaled = key * learn
    taken = unit * learn
    back = jnp.sum(taken * recept, axis=-1, keepdims=True)
    fresh = jnp.sum(scaled * recept, axis=-1, keepdims=True)
    probe = forget * recept - back * unit

    def twice(t):
        return jnp.concatenate([t, t], axis=1)

    halves, place = masks(pairs, head)
    probe = twice(probe)
    folded = []
    for n in range(steps):
        copies[n].wait()
        at = slice(n * block, (n + 1) * block)
        product = (s_ref[at] * probe[at][:, None, :]).reshape(block * pairs, LANES)
        sums = half_sums(product, halves).reshape(block, pairs, LANES)
        folded.append(jnp.sum(sums * place[None], axis=1))
    folded = jnp.concatenate(folded, axis=0)
    read = folded[:, :head] + folded[:, head:] + value * fresh
    centre = read - jnp.mean(read, axis=-1, keepdims=True)
    normal = centre * lax.rsqrt(jnp.mean(centre * centre, axis=-1, keepdims=True) + group_floor)
    mixed_ref[...] = (normal * gain_ref[layer:layer + 1, :] * jax.nn.sigmoid(gate)).astype(BF16)
    vec_ref[...] = jnp.concatenate(
        [twice(forget), twice(-unit), twice(taken), twice(value), twice(scaled)], axis=1)


def update_body(*refs, head):
    vec_ref, s_ref, out_ref = refs[0], refs[1], refs[-1]
    rows, pairs, _ = s_ref.shape
    forget, away, taken, value, scaled = (
        vec_ref[:, n * LANES:(n + 1) * LANES][:, None, :] for n in range(5))
    halves, place = masks(pairs, head)
    state = s_ref[...]
    removed = half_sums((state * away).reshape(rows * pairs, LANES), halves)
    spread = (value * place[None]).reshape(rows * pairs, LANES).astype(BF16)
    values = jnp.dot(spread, halves, preferred_element_type=F32)
    shape = (rows, pairs, LANES)
    out_ref[...] = state * forget + removed.reshape(shape) * taken + values.reshape(shape) * scaled


def output_body(pos_ref, *refs, outer, inner):
    m_refs, w_refs = refs[:outer], refs[outer:2 * outer]
    own_ref, sends = refs[2 * outer], refs[2 * outer + 1:-1]
    acc = refs[-1]
    left = jnp.concatenate([m[...] for m in m_refs], axis=1)
    right = jnp.concatenate([w[...] for w in w_refs], axis=0)
    acc[...] = jnp.dot(left, right, preferred_element_type=F32)
    width = own_ref.shape[1]
    for b in range(inner):
        at = pl.ds(pl.multiple_of((pos_ref[2] ^ b) * width, LANES), width)
        if b == 0:
            own_ref[...] = acc[:, at]
        else:
            sends[b - 1][...] = acc[:, at].astype(BF16)


def assemble_body(pos_ref, *refs):
    out_ref, inner = refs[-1], len(refs) - 1
    rows = out_ref.shape[0] // 2
    for b in range(inner):
        for a in range(refs[b].shape[0]):
            chunk = (pos_ref[1] ^ a) * inner + (pos_ref[2] ^ b)
            width = refs[b].shape[2]
            at = pl.ds(pl.multiple_of(chunk * width, LANES), width)
            for half in range(2):
                row = pl.multiple_of((pos_ref[0] ^ half) * rows, 16)
                out_ref[pl.ds(row, rows), at] = refs[b][a, half * rows:(half + 1) * rows, :]


SMEM = functools.partial(pl.BlockSpec, memory_space=pltpu.SMEM)
VMEM = functools.partial(pl.BlockSpec, memory_space=pltpu.VMEM)


def vmem(*arrays):
    return [pltpu.with_memory_space_constraint(a, pltpu.VMEM) for a in arrays]


def whole(shape):
    return VMEM()


def shards(tp, dp, tokens, norm_gain, receptance, key_proj, value_proj, decay_proj, rate_proj,
           gate_proj, decay_base, group_gain, output_proj, state):
    inner = 4 if tp % 4 == 0 else tp
    outer = tp // inner
    layers, rows, _, cells = state.shape
    batch, local_width = tokens.shape
    head = decay_base.shape[1]
    pairs = cells // LANES
    width = local_width * dp
    me = lax.axis_index("tp")
    pos = jnp.stack([lax.axis_index("dp"), me // inner, me % inner]).astype(jnp.int32)
    far, near = me // inner, me % inner

    def over_far(t, s):
        return lax.ppermute(t, "tp", [(i, ((i // inner) ^ s) * inner + i % inner) for i in range(tp)])

    def over_near(t, s):
        return lax.ppermute(t, "tp", [(i, (i // inner) * inner + ((i % inner) ^ s)) for i in range(tp)])

    def swap(t):
        return lax.ppermute(t, "dp", [(i, i ^ 1) for i in range(dp)])

    projections = [jnp.swapaxes(w, 1, 2) for w in (
        receptance, key_proj, value_proj, decay_proj, rate_proj, gate_proj)]
    states = state.reshape(layers, rows, pairs, LANES)

    band = local_width // outer
    chunk = band // inner
    bands = [lax.dynamic_slice_in_dim(output_proj, (far ^ s) * band, band, 2) for s in range(outer)]
    out_weights = [bands[0]] + [over_far(bands[s], s) for s in range(1, outer)]

    current = jnp.concatenate(
        [lax.dynamic_slice(tokens, (row, me * chunk), (rows, chunk))
         for row in (pos[0] * rows, (1 - pos[0]) * rows)], axis=0)
    gathered = (tokens,)
    new_states = None
    block = rows // 4
    vec_width = 5 * LANES
    for layer in range(layers):
        first = len(gathered) == 1
        sums_width = 6 * head + LANES
        own, other = pl.pallas_call(
            functools.partial(project_body, count=len(gathered), layer=layer, heads_width=head),
            in_specs=[SMEM()] + [whole(g.shape) for g in gathered] + [VMEM()]
            + [pl.BlockSpec(memory_space=pl.ANY)] * (6 if first else 7),
            out_specs=[whole((rows, sums_width))] * 2,
            out_shape=[pltpu.VMEM((rows, sums_width), F32)] * 2,
            scratch_shapes=[pltpu.VMEM((batch, local_width), BF16), pltpu.VMEM((batch, sums_width), F32),
                            pltpu.VMEM((6 * head, local_width), BF16), pltpu.SemaphoreType.DMA((6,))],
            name=f"project{layer}",
            cost_estimate=COST,
        )(pos, *(gathered if first else vmem(*gathered)), norm_gain, *projections,
          *([] if first else [new_states]))
        received = swap(other)

        def row_block(w):
            return pl.BlockSpec((block, w), lambda i: (i, 0))

        state_block = pl.BlockSpec(
            (None, block, pairs, LANES), lambda i, layer=layer: (layer, i, 0, 0))
        mixed, vectors = pl.pallas_call(
            functools.partial(head_body, layer=layer, head=head, width=width),
            in_specs=[VMEM()] * 4 + [pl.BlockSpec(memory_space=pl.ANY)],
            out_specs=[VMEM()] * 2,
            scratch_shapes=[pltpu.VMEM(states.shape[1:], F32), pltpu.SemaphoreType.DMA((8,))],
            out_shape=[pltpu.VMEM((rows, head), BF16),
                       jax.ShapeDtypeStruct((rows, vec_width), F32)],
            name=f"heads{layer}",
            cost_estimate=COST,
        )(*vmem(own, received), decay_base, group_gain, states)

        partner = swap(mixed)
        both = jnp.concatenate([mixed, partner], axis=0)
        columns = [both] + [over_far(both, s) for s in range(1, outer)]

        previous = [] if new_states is None else [new_states]
        new_states = pl.pallas_call(
            functools.partial(update_body, head=head),
            grid=(4,),
            in_specs=[row_block(vec_width), state_block]
            + [pl.BlockSpec(memory_space=pl.ANY)] * len(previous),
            out_specs=state_block,
            out_shape=jax.ShapeDtypeStruct(states.shape, F32),
            input_output_aliases={2: 0} if previous else {},
            name=f"update{layer}",
            cost_estimate=COST,
        )(vectors, states, *previous)

        weights = [w[layer] for w in out_weights]
        mine, *sends = pl.pallas_call(
            functools.partial(output_body, outer=outer, inner=inner),
            in_specs=[SMEM()] + [whole(c.shape) for c in columns] + [whole(w.shape) for w in weights],
            out_specs=[whole((batch, chunk))] * inner,
            out_shape=[pltpu.VMEM((batch, chunk), F32)]
            + [pltpu.VMEM((batch, chunk), BF16)] * (inner - 1),
            scratch_shapes=[pltpu.VMEM((batch, band), F32)],
            name=f"output{layer}",
            cost_estimate=COST,
        )(pos, *vmem(*columns, *weights))
        total = current.astype(F32) + mine
        for s in range(1, inner):
            total = total + over_near(sends[s - 1], s).astype(F32)
        current = total.astype(BF16)
        stack = jnp.stack([current] + [over_far(current, s) for s in range(1, outer)])
        gathered = (stack,) + tuple(over_near(stack, s) for s in range(1, inner))

    final = pl.pallas_call(
        assemble_body,
        in_specs=[SMEM()] + [whole(g.shape) for g in gathered],
        out_specs=whole((batch, local_width)),
        out_shape=jax.ShapeDtypeStruct((batch, local_width), BF16),
        name="assemble",
        cost_estimate=COST,
    )(pos, *vmem(*gathered))
    return final, new_states.reshape(state.shape)


def recurrence(state_block, recept_heads, key_heads, value_heads, decay_heads, rate_heads):
    log_rate = -jax.nn.softplus(-decay_heads) - 0.5
    forget = jnp.exp(-jnp.exp(log_rate))
    learn_rate = jax.nn.sigmoid(rate_heads)
    unit_key = key_heads * lax.rsqrt(jnp.sum(key_heads * key_heads, axis=-1, keepdims=True) + 1.0)
    scaled = key_heads * learn_rate
    removed = jnp.einsum("bhvk,bhk->bhv", state_block, -unit_key, precision=lax.Precision.HIGHEST)
    updated = (
        state_block * forget[:, :, None, :]
        + removed[..., None] * (unit_key * learn_rate)[:, :, None, :]
        + value_heads[..., None] * scaled[:, :, None, :]
    )
    read_out = jnp.einsum("bhvk,bhk->bhv", updated, recept_heads, precision=lax.Precision.HIGHEST)
    centre = read_out - jnp.mean(read_out, axis=-1, keepdims=True)
    normal = centre * lax.rsqrt(jnp.mean(centre * centre, axis=-1, keepdims=True) + group_floor)
    return (updated, normal)


def plain_shards(
    tokens,
    norm_gain,
    receptance,
    key_proj,
    value_proj,
    decay_proj,
    rate_proj,
    gate_proj,
    decay_base,
    group_gain,
    output_proj,
    state,
):
    local_rows = state.shape[1]
    first_row = lax.axis_index("dp") * local_rows
    local_heads = state.shape[2]
    current = tokens
    width = tokens.shape[1] * lax.psum(1, "dp")
    head = decay_base.shape[1] // local_heads
    finals = []
    for section_index in range(state.shape[0]):
        floats = current.astype(jnp.float32)
        squares = jnp.sum(floats * floats, axis=1)
        normed = (floats * norm_gain[section_index]).astype(jnp.bfloat16)
        part_recept = jnp.dot(normed, receptance[section_index], preferred_element_type=jnp.float32)
        part_key = jnp.dot(normed, key_proj[section_index], preferred_element_type=jnp.float32)
        part_value = jnp.dot(normed, value_proj[section_index], preferred_element_type=jnp.float32)
        part_decay = jnp.dot(normed, decay_proj[section_index], preferred_element_type=jnp.float32)
        part_rate = jnp.dot(normed, rate_proj[section_index], preferred_element_type=jnp.float32)
        part_gate = jnp.dot(normed, gate_proj[section_index], preferred_element_type=jnp.float32)
        totals = lax.psum(squares, "dp")
        own_squares = lax.dynamic_slice_in_dim(totals, first_row, local_rows, 0)
        summed = (
            lax.psum_scatter(part_recept, "dp", scatter_dimension=0, tiled=True),
            lax.psum_scatter(part_key, "dp", scatter_dimension=0, tiled=True),
            lax.psum_scatter(part_value, "dp", scatter_dimension=0, tiled=True),
            lax.psum_scatter(part_decay, "dp", scatter_dimension=0, tiled=True),
            lax.psum_scatter(part_rate, "dp", scatter_dimension=0, tiled=True),
            lax.psum_scatter(part_gate, "dp", scatter_dimension=0, tiled=True),
        )
        inv_rms = lax.rsqrt(own_squares / width + norm_floor)

        def by_head(term):
            rounded = lax.optimization_barrier((inv_rms[:, None] * term).astype(jnp.bfloat16))
            return rounded.astype(jnp.float32).reshape(local_rows, local_heads, head)

        decay_heads = by_head(summed[3]) + decay_base[section_index].reshape(1, local_heads, head)
        updated, normal = recurrence(
            state[section_index].reshape(local_rows, local_heads, head, head),
            by_head(summed[0]),
            by_head(summed[1]),
            by_head(summed[2]),
            decay_heads,
            by_head(summed[4]),
        )
        finals.append(updated.reshape(local_rows, local_heads, state.shape[3]))
        gate_value = jax.nn.sigmoid(by_head(summed[5]).reshape(local_rows, local_heads * head))
        mixed_heads = (
            normal.reshape(local_rows, local_heads * head) * group_gain[section_index] * gate_value
        ).astype(jnp.bfloat16)
        weights_out = output_proj[section_index]

        def apply_out(piece, begin, weights_out=weights_out):
            return jnp.dot(piece, weights_out, preferred_element_type=jnp.float32)

        partial_out = apply_out(lax.all_gather(mixed_heads, "dp", axis=0, tiled=True), jnp.int32(0))
        total = lax.psum(partial_out, "tp")
        current = (floats + total).astype(jnp.bfloat16)
    return (current, jnp.stack(finals))


def solution(mesh):
    tp, dp = mesh.shape["tp"], mesh.shape["dp"]

    def body(*args):
        tokens, decay_base, state = args[0], args[8], args[11]
        chunks = tokens.shape[1] % (tp * LANES) == 0 and decay_base.shape[1] * 2 == LANES
        blocks = state.shape[1] % 64 == 0 and state.shape[2] == 1
        if dp == 2 and tp & (tp - 1) == 0 and tp % 4 == 0 and chunks and blocks:
            return shards(tp, dp, *args)
        return plain_shards(*args)

    return jax.shard_map(
        body,
        mesh=mesh,
        in_specs=(
            P(None, "dp"),
            P(None, "dp"),
            P(None, "dp", "tp"),
            P(None, "dp", "tp"),
            P(None, "dp", "tp"),
            P(None, "dp", "tp"),
            P(None, "dp", "tp"),
            P(None, "dp", "tp"),
            P(None, "tp"),
            P(None, "tp"),
            P(None, "tp", "dp"),
            P(None, "dp", "tp", None),
        ),
        out_specs=(P(None, "dp"), P(None, "dp", "tp", None)),
        check_vma=False,
    )
```

```python
import functools

import jax
import jax.numpy as jnp
from jax import lax
from jax.experimental import pallas as pl
from jax.experimental.pallas import tpu as pltpu
from jax.sharding import PartitionSpec as P

LANES = 128
norm_floor = 0.1
group_floor = 0.5
F32, BF16 = jnp.float32, jnp.bfloat16

COST = pl.CostEstimate(flops=20_000_000, transcendentals=0, bytes_accessed=8_000_000)


def project_body(pos_ref, *refs, count, layer, heads_width):
    x_refs, (gain_ref, *w_refs), (own_ref, other_ref), (normed, acc, weights, arrived) = (
        refs[:count], refs[count:count + 7], refs[-6:-4], refs[-4:])
    copies = [pltpu.make_async_copy(
        w.at[layer], weights.at[pl.ds(n * heads_width, heads_width)], arrived.at[n])
        for n, w in enumerate(w_refs)]
    for copy in copies:
        copy.start()
    squares = jnp.zeros((acc.shape[0], 1), F32)
    if count == 1:
        floats = x_refs[0][...].astype(F32)
        squares = jnp.sum(floats * floats, axis=1, keepdims=True)
        normed[...] = (floats * gain_ref[layer:layer + 1, :]).astype(BF16)
    else:
        inner = count
        for b in range(inner):
            for a in range(x_refs[b].shape[0]):
                chunk = (pos_ref[1] ^ a) * inner + (pos_ref[2] ^ b)
                width = x_refs[b].shape[2]
                at = pl.ds(pl.multiple_of(chunk * width, LANES), width)
                floats = x_refs[b][a].astype(F32)
                squares = squares + jnp.sum(floats * floats, axis=1, keepdims=True)
                normed[:, at] = (floats * gain_ref[layer:layer + 1, at]).astype(BF16)
    for copy in copies:
        copy.wait()
    acc[:, :6 * heads_width] = lax.dot_general(
        normed[...], weights[...], (((1,), (1,)), ((), ())), preferred_element_type=F32)
    acc[:, 6 * heads_width:] = jnp.broadcast_to(squares, (acc.shape[0], LANES))
    rows = own_ref.shape[0]
    if count == 1:
        core = pos_ref[0]
        own_ref[...] = acc[pl.ds(pl.multiple_of(core * rows, 8), rows), :]
        other_ref[...] = acc[pl.ds(pl.multiple_of((1 - core) * rows, 8), rows), :]
    else:
        own_ref[...] = acc[:rows, :]
        other_ref[...] = acc[rows:, :]


def masks(pairs, head):
    i = lax.broadcasted_iota(jnp.int32, (LANES, LANES), 0)
    j = lax.broadcasted_iota(jnp.int32, (LANES, LANES), 1)
    halves = jnp.where((i // head) == (j // head), 1.0, 0.0).astype(BF16)
    s = lax.broadcasted_iota(jnp.int32, (pairs, LANES), 0)
    lane = lax.broadcasted_iota(jnp.int32, (pairs, LANES), 1)
    place = jnp.where((lane == 2 * s) | (lane == head + 2 * s + 1), 1.0, 0.0)
    return halves, place


def half_sums(product, halves):
    high = product.astype(BF16)
    low = (product - high.astype(F32)).astype(BF16)
    return (jnp.dot(high, halves, preferred_element_type=F32)
            + jnp.dot(low, halves, preferred_element_type=F32))


def head_body(own_ref, recv_ref, base_ref, gain_ref, s_hbm, mixed_ref, vec_ref, s_ref, arrived,
              *, layer, head, width):
    rows, pairs, _ = s_ref.shape
    steps = arrived.shape[0]
    block = rows // steps
    copies = [pltpu.make_async_copy(
        s_hbm.at[layer, pl.ds(n * block, block)], s_ref.at[pl.ds(n * block, block)], arrived.at[n])
        for n in range(steps)]
    for copy in copies:
        copy.start()
    total = own_ref[...] + recv_ref[...]
    inv_rms = lax.rsqrt(total[:, 6 * head:6 * head + 1] / width + norm_floor)
    seen = (total[:, :6 * head] * inv_rms).astype(BF16).astype(F32)
    recept, key, value, decay, rate, gate = (seen[:, n * head:(n + 1) * head] for n in range(6))
    forget = jnp.exp(-jnp.exp(jnp.float32(-0.5)) * jax.nn.sigmoid(decay + base_ref[layer:layer + 1, :]))
    learn = jax.nn.sigmoid(rate)
    unit = key * lax.rsqrt(jnp.sum(key * key, axis=-1, keepdims=True) + 1.0)
    scaled = key * learn
    taken = unit * learn
    back = jnp.sum(taken * recept, axis=-1, keepdims=True)
    fresh = jnp.sum(scaled * recept, axis=-1, keepdims=True)
    probe = forget * recept - back * unit

    def twice(t):
        return jnp.concatenate([t, t], axis=1)

    halves, place = masks(pairs, head)
    probe = twice(probe)
    folded = []
    for n in range(steps):
        copies[n].wait()
        at = slice(n * block, (n + 1) * block)
        product = (s_ref[at] * probe[at][:, None, :]).reshape(block * pairs, LANES)
        sums = half_sums(product, halves).reshape(block, pairs, LANES)
        folded.append(jnp.sum(sums * place[None], axis=1))
    folded = jnp.concatenate(folded, axis=0)
    read = folded[:, :head] + folded[:, head:] + value * fresh
    centre = read - jnp.mean(read, axis=-1, keepdims=True)
    normal = centre * lax.rsqrt(jnp.mean(centre * centre, axis=-1, keepdims=True) + group_floor)
    mixed_ref[...] = (normal * gain_ref[layer:layer + 1, :] * jax.nn.sigmoid(gate)).astype(BF16)
    vec_ref[...] = jnp.concatenate(
        [twice(forget), twice(-unit), twice(taken), twice(value), twice(scaled)], axis=1)


def update_body(*refs, head):
    vec_ref, s_ref, out_ref = refs[0], refs[1], refs[-1]
    rows, pairs, _ = s_ref.shape
    forget, away, taken, value, scaled = (
        vec_ref[:, n * LANES:(n + 1) * LANES][:, None, :] for n in range(5))
    halves, place = masks(pairs, head)
    state = s_ref[...]
    removed = half_sums((state * away).reshape(rows * pairs, LANES), halves)
    spread = (value * place[None]).reshape(rows * pairs, LANES).astype(BF16)
    values = jnp.dot(spread, halves, preferred_element_type=F32)
    shape = (rows, pairs, LANES)
    out_ref[...] = state * forget + removed.reshape(shape) * taken + values.reshape(shape) * scaled


def output_body(pos_ref, *refs, outer, inner):
    m_refs, w_refs = refs[:outer], refs[outer:2 * outer]
    own_ref, sends = refs[2 * outer], refs[2 * outer + 1:-1]
    acc = refs[-1]
    left = jnp.concatenate([m[...] for m in m_refs], axis=1)
    right = jnp.concatenate([w[...] for w in w_refs], axis=0)
    acc[...] = jnp.dot(left, right, preferred_element_type=F32)
    width = own_ref.shape[1]
    for b in range(inner):
        at = pl.ds(pl.multiple_of((pos_ref[2] ^ b) * width, LANES), width)
        if b == 0:
            own_ref[...] = acc[:, at]
        else:
            sends[b - 1][...] = acc[:, at].astype(BF16)


def assemble_body(pos_ref, *refs):
    out_ref, inner = refs[-1], len(refs) - 1
    rows = out_ref.shape[0] // 2
    for b in range(inner):
        for a in range(refs[b].shape[0]):
            chunk = (pos_ref[1] ^ a) * inner + (pos_ref[2] ^ b)
            width = refs[b].shape[2]
            at = pl.ds(pl.multiple_of(chunk * width, LANES), width)
            for half in range(2):
                row = pl.multiple_of((pos_ref[0] ^ half) * rows, 16)
                out_ref[pl.ds(row, rows), at] = refs[b][a, half * rows:(half + 1) * rows, :]


SMEM = functools.partial(pl.BlockSpec, memory_space=pltpu.SMEM)
VMEM = functools.partial(pl.BlockSpec, memory_space=pltpu.VMEM)


def vmem(*arrays):
    return [pltpu.with_memory_space_constraint(a, pltpu.VMEM) for a in arrays]


def whole(shape):
    return VMEM()


def shards(tp, dp, tokens, norm_gain, receptance, key_proj, value_proj, decay_proj, rate_proj,
           gate_proj, decay_base, group_gain, output_proj, state):
    inner = 4 if tp % 4 == 0 else tp
    outer = tp // inner
    layers, rows, _, cells = state.shape
    batch, local_width = tokens.shape
    head = decay_base.shape[1]
    pairs = cells // LANES
    width = local_width * dp
    me = lax.axis_index("tp")
    pos = jnp.stack([lax.axis_index("dp"), me // inner, me % inner]).astype(jnp.int32)
    far, near = me // inner, me % inner

    def over_far(t, s):
        return lax.ppermute(t, "tp", [(i, ((i // inner) ^ s) * inner + i % inner) for i in range(tp)])

    def over_near(t, s):
        return lax.ppermute(t, "tp", [(i, (i // inner) * inner + ((i % inner) ^ s)) for i in range(tp)])

    def swap(t):
        return lax.ppermute(t, "dp", [(i, i ^ 1) for i in range(dp)])

    projections = [jnp.swapaxes(w, 1, 2) for w in (
        receptance, key_proj, value_proj, decay_proj, rate_proj, gate_proj)]
    states = state.reshape(layers, rows, pairs, LANES)

    band = local_width // outer
    chunk = band // inner
    current = jnp.concatenate(
        [lax.dynamic_slice(tokens, (row, me * chunk), (rows, chunk))
         for row in (pos[0] * rows, (1 - pos[0]) * rows)], axis=0)
    gathered = (tokens,)
    new_states = None
    block = rows // 4
    vec_width = 5 * LANES
    for layer in range(layers):
        first = len(gathered) == 1
        sums_width = 6 * head + LANES
        own, other = pl.pallas_call(
            functools.partial(project_body, count=len(gathered), layer=layer, heads_width=head),
            in_specs=[SMEM()] + [whole(g.shape) for g in gathered] + [VMEM()]
            + [pl.BlockSpec(memory_space=pl.ANY)] * (6 if first else 7),
            out_specs=[whole((rows, sums_width))] * 2,
            out_shape=[pltpu.VMEM((rows, sums_width), F32)] * 2,
            scratch_shapes=[pltpu.VMEM((batch, local_width), BF16), pltpu.VMEM((batch, sums_width), F32),
                            pltpu.VMEM((6 * head, local_width), BF16), pltpu.SemaphoreType.DMA((6,))],
            name=f"project{layer}",
            cost_estimate=COST,
        )(pos, *(gathered if first else vmem(*gathered)), norm_gain, *projections,
          *([] if first else [new_states]))
        if first:
            output_proj, other = lax.optimization_barrier((output_proj, other))
            bands = [lax.dynamic_slice_in_dim(output_proj, (far ^ s) * band, band, 2) for s in range(outer)]
            out_weights = [bands[0]] + [over_far(bands[s], s) for s in range(1, outer)]
        received = swap(other)

        def row_block(w):
            return pl.BlockSpec((block, w), lambda i: (i, 0))

        state_block = pl.BlockSpec(
            (None, block, pairs, LANES), lambda i, layer=layer: (layer, i, 0, 0))
        mixed, vectors = pl.pallas_call(
            functools.partial(head_body, layer=layer, head=head, width=width),
            in_specs=[VMEM()] * 4 + [pl.BlockSpec(memory_space=pl.ANY)],
            out_specs=[VMEM()] * 2,
            scratch_shapes=[pltpu.VMEM(states.shape[1:], F32), pltpu.SemaphoreType.DMA((8,))],
            out_shape=[pltpu.VMEM((rows, head), BF16),
                       jax.ShapeDtypeStruct((rows, vec_width), F32)],
            name=f"heads{layer}",
            cost_estimate=COST,
        )(*vmem(own, received), decay_base, group_gain, states)

        partner = swap(mixed)
        both = jnp.concatenate([mixed, partner], axis=0)
        columns = [both] + [over_far(both, s) for s in range(1, outer)]

        previous = [] if new_states is None else [new_states]
        new_states = pl.pallas_call(
            functools.partial(update_body, head=head),
            grid=(4,),
            in_specs=[row_block(vec_width), state_block]
            + [pl.BlockSpec(memory_space=pl.ANY)] * len(previous),
            out_specs=state_block,
            out_shape=jax.ShapeDtypeStruct(states.shape, F32),
            input_output_aliases={2: 0} if previous else {},
            name=f"update{layer}",
            cost_estimate=COST,
        )(vectors, states, *previous)

        weights = [w[layer] for w in out_weights]
        mine, *sends = pl.pallas_call(
            functools.partial(output_body, outer=outer, inner=inner),
            in_specs=[SMEM()] + [whole(c.shape) for c in columns] + [whole(w.shape) for w in weights],
            out_specs=[whole((batch, chunk))] * inner,
            out_shape=[pltpu.VMEM((batch, chunk), F32)]
            + [pltpu.VMEM((batch, chunk), BF16)] * (inner - 1),
            scratch_shapes=[pltpu.VMEM((batch, band), F32)],
            name=f"output{layer}",
            cost_estimate=COST,
        )(pos, *vmem(*columns, *weights))
        total = current.astype(F32) + mine
        for s in range(1, inner):
            total = total + over_near(sends[s - 1], s).astype(F32)
        current = total.astype(BF16)
        stack = jnp.stack([current] + [over_far(current, s) for s in range(1, outer)])
        gathered = (stack,) + tuple(over_near(stack, s) for s in range(1, inner))

    final = pl.pallas_call(
        assemble_body,
        in_specs=[SMEM()] + [whole(g.shape) for g in gathered],
        out_specs=whole((batch, local_width)),
        out_shape=jax.ShapeDtypeStruct((batch, local_width), BF16),
        name="assemble",
        cost_estimate=COST,
    )(pos, *vmem(*gathered))
    return final, new_states.reshape(state.shape)


def recurrence(state_block, recept_heads, key_heads, value_heads, decay_heads, rate_heads):
    log_rate = -jax.nn.softplus(-decay_heads) - 0.5
    forget = jnp.exp(-jnp.exp(log_rate))
    learn_rate = jax.nn.sigmoid(rate_heads)
    unit_key = key_heads * lax.rsqrt(jnp.sum(key_heads * key_heads, axis=-1, keepdims=True) + 1.0)
    scaled = key_heads * learn_rate
    removed = jnp.einsum("bhvk,bhk->bhv", state_block, -unit_key, precision=lax.Precision.HIGHEST)
    updated = (
        state_block * forget[:, :, None, :]
        + removed[..., None] * (unit_key * learn_rate)[:, :, None, :]
        + value_heads[..., None] * scaled[:, :, None, :]
    )
    read_out = jnp.einsum("bhvk,bhk->bhv", updated, recept_heads, precision=lax.Precision.HIGHEST)
    centre = read_out - jnp.mean(read_out, axis=-1, keepdims=True)
    normal = centre * lax.rsqrt(jnp.mean(centre * centre, axis=-1, keepdims=True) + group_floor)
    return (updated, normal)


def plain_shards(
    tokens,
    norm_gain,
    receptance,
    key_proj,
    value_proj,
    decay_proj,
    rate_proj,
    gate_proj,
    decay_base,
    group_gain,
    output_proj,
    state,
):
    local_rows = state.shape[1]
    first_row = lax.axis_index("dp") * local_rows
    local_heads = state.shape[2]
    current = tokens
    width = tokens.shape[1] * lax.psum(1, "dp")
    head = decay_base.shape[1] // local_heads
    finals = []
    for section_index in range(state.shape[0]):
        floats = current.astype(jnp.float32)
        squares = jnp.sum(floats * floats, axis=1)
        normed = (floats * norm_gain[section_index]).astype(jnp.bfloat16)
        part_recept = jnp.dot(normed, receptance[section_index], preferred_element_type=jnp.float32)
        part_key = jnp.dot(normed, key_proj[section_index], preferred_element_type=jnp.float32)
        part_value = jnp.dot(normed, value_proj[section_index], preferred_element_type=jnp.float32)
        part_decay = jnp.dot(normed, decay_proj[section_index], preferred_element_type=jnp.float32)
        part_rate = jnp.dot(normed, rate_proj[section_index], preferred_element_type=jnp.float32)
        part_gate = jnp.dot(normed, gate_proj[section_index], preferred_element_type=jnp.float32)
        totals = lax.psum(squares, "dp")
        own_squares = lax.dynamic_slice_in_dim(totals, first_row, local_rows, 0)
        summed = (
            lax.psum_scatter(part_recept, "dp", scatter_dimension=0, tiled=True),
            lax.psum_scatter(part_key, "dp", scatter_dimension=0, tiled=True),
            lax.psum_scatter(part_value, "dp", scatter_dimension=0, tiled=True),
            lax.psum_scatter(part_decay, "dp", scatter_dimension=0, tiled=True),
            lax.psum_scatter(part_rate, "dp", scatter_dimension=0, tiled=True),
            lax.psum_scatter(part_gate, "dp", scatter_dimension=0, tiled=True),
        )
        inv_rms = lax.rsqrt(own_squares / width + norm_floor)

        def by_head(term):
            rounded = lax.optimization_barrier((inv_rms[:, None] * term).astype(jnp.bfloat16))
            return rounded.astype(jnp.float32).reshape(local_rows, local_heads, head)

        decay_heads = by_head(summed[3]) + decay_base[section_index].reshape(1, local_heads, head)
        updated, normal = recurrence(
            state[section_index].reshape(local_rows, local_heads, head, head),
            by_head(summed[0]),
            by_head(summed[1]),
            by_head(summed[2]),
            decay_heads,
            by_head(summed[4]),
        )
        finals.append(updated.reshape(local_rows, local_heads, state.shape[3]))
        gate_value = jax.nn.sigmoid(by_head(summed[5]).reshape(local_rows, local_heads * head))
        mixed_heads = (
            normal.reshape(local_rows, local_heads * head) * group_gain[section_index] * gate_value
        ).astype(jnp.bfloat16)
        weights_out = output_proj[section_index]

        def apply_out(piece, begin, weights_out=weights_out):
            return jnp.dot(piece, weights_out, preferred_element_type=jnp.float32)

        partial_out = apply_out(lax.all_gather(mixed_heads, "dp", axis=0, tiled=True), jnp.int32(0))
        total = lax.psum(partial_out, "tp")
        current = (floats + total).astype(jnp.bfloat16)
    return (current, jnp.stack(finals))


def solution(mesh):
    tp, dp = mesh.shape["tp"], mesh.shape["dp"]

    def body(*args):
        tokens, decay_base, state = args[0], args[8], args[11]
        chunks = tokens.shape[1] % (tp * LANES) == 0 and decay_base.shape[1] * 2 == LANES
        blocks = state.shape[1] % 64 == 0 and state.shape[2] == 1
        if dp == 2 and tp & (tp - 1) == 0 and tp % 4 == 0 and chunks and blocks:
            return shards(tp, dp, *args)
        return plain_shards(*args)

    return jax.shard_map(
        body,
        mesh=mesh,
        in_specs=(
            P(None, "dp"),
            P(None, "dp"),
            P(None, "dp", "tp"),
            P(None, "dp", "tp"),
            P(None, "dp", "tp"),
            P(None, "dp", "tp"),
            P(None, "dp", "tp"),
            P(None, "dp", "tp"),
            P(None, "tp"),
            P(None, "tp"),
            P(None, "tp", "dp"),
            P(None, "dp", "tp", None),
        ),
        out_specs=(P(None, "dp"), P(None, "dp", "tp", None)),
        check_vma=False,
    )
```
